32 devices in a mesh: sp: 8 (over z, y), tp: 4 (over x, core).
Axes of the slice: x: 2, y: 2, z: 4, core: 2. Of those that a mesh axis runs over, the one named last changes fastest.
Arguments:
- expert_input: bfloat16 [3072, 2048], P('sp'), may hold values from -6 to 6
- cotangent: bfloat16 [3072, 2048], P('sp'), may hold values from -6 to 6
- routes: int32 [3072, 2], P('sp'), may hold values from 0 to 7, all different within a row; in each aligned block of 384 rows (0 to 383, 384 to 767, ...) at most 144 rows name the same one
- route_weight: float32 [3072, 2], P('sp'), may hold values from 0.2 to 2.5
- expert_gate: bfloat16 [8, 2048, 1024], P('sp', None, 'tp'), may hold values from -0.125 to 0.125
- expert_up: bfloat16 [8, 2048, 1024], P('sp', None, 'tp'), may hold values from -0.125 to 0.125
- expert_down: bfloat16 [8, 1024, 2048], P('sp', 'tp'), may hold values from -0.1875 to 0.1875
- conv_out: bfloat16 [3072, 1024], P('sp', 'tp'), may hold values from -14 to 14
- conv_value: bfloat16 [3072, 1024], P('sp', 'tp'), may hold values from -6 to 6
- conv_gate: bfloat16 [3072, 1024], P('sp', 'tp'), may hold values from -6 to 6
- conv_taps: float32 [31, 1024], P(None, 'tp'), may hold values from -1 to 1
- norm_gain: float32 [1024], P('tp'), may hold values from 0.1 to 1.9
- norm_bias: float32 [1024], P('tp'), may hold values from -3 to 3
- out_weight: bfloat16 [1024, 2048], P('tp'), may hold values from -0.1875 to 0.1875
Outputs:
- gate_grad: float32 [8, 2048, 1024], P('sp', None, 'tp')
- up_grad: float32 [8, 2048, 1024], P('sp', None, 'tp')
- down_grad: float32 [8, 1024, 2048], P('sp', 'tp')
- resid_grad: bfloat16 [3072, 2048], P('sp')
- out_weight_grad: float32 [1024, 2048], P('tp', 'sp')
- value_grad: bfloat16 [3072, 1024], P('sp', 'tp')
- gate_in_grad: bfloat16 [3072, 1024], P('sp', 'tp')
The draws below stay inside these ranges and needn't reach their ends.
Inputs may be any that keep to these rules, and one draw needn't show every extreme that they name: `routes`: each token names 2 different experts. In each aligned block of 384 tokens no expert is named by more than 144 tokens, and in every draw some block has an expert named by exactly 144 tokens.
All inputs are finite; a program needn't handle non-finite values.
Results may differ from the reference program's by a relative error of at most 0.018.
Values may be sent and summed in bfloat16 or wider, within the bound.
A program may use at most 128 MiB of HBM per device.

```python
import math
import jax
import jax.numpy as jnp
import numpy as np
from jax import lax

D = 2048
CW = 1024
FF = 1024
KW = 31
TOP = 2
TOK_DEV = 384
TOKENS = 3072
EXPERTS = 8
CAP = 144
FGROUP = 256
N_SP = 8
N_TP = 4


def draw_conv_out(key, part):
    first_key = jax.random.fold_in(jax.random.fold_in(key, 11), 0)
    column = jnp.arange(CW, dtype=jnp.float32) / CW
    col_scale = 0.3 * jnp.exp(jnp.log(10.0) * column)[None, :]
    values = jnp.clip(jax.random.normal(first_key, (TOKENS, CW), jnp.float32), -4.0, 4.0) * col_scale
    return values.astype(jnp.bfloat16)


def spiked(array, rng, source, target, parts, factor):
    def block_of(axis_at):
        return (jnp.arange(array.shape[axis_at]) // (array.shape[axis_at] // parts)).reshape((-1,) + (1,) * (array.ndim - 1 - axis_at))

    near = jax.random.permutation(rng, parts)[block_of(target)]
    other_side = (block_of(target) + parts // 2) % parts
    return jnp.where((block_of(source) == near) | (block_of(source) == other_side), factor * array, array)


def levels(stream_key, dims, pieces, low, largest):
    loudness, own = 1.0, jax.random.fold_in(stream_key, 6)
    for position, parts in pieces:
        steps = jnp.exp(jax.random.uniform(jax.random.fold_in(own, position), (parts,), jnp.float32, low / len(pieces), largest / len(pieces)))
        loudness = loudness * jnp.repeat(steps, dims[position] // parts).reshape([-1 if axis == position else 1 for axis in range(len(dims))])
    return loudness


def assign_block(rng, own, number, rows, number_of, top, most, skew):
    order = jax.random.permutation(rng, number_of)
    crowded, usual = load_shares(number_of, rows * top, most, skew, True), load_shares(number_of, rows * top, most, skew, False)
    places = jnp.arange(number_of)

    def named(tallies, rotation):
        used = int((tallies > 0).sum())
        fixed = max(1, used // 4)
        moved = fixed + (places - fixed + rotation * (used - fixed)) % max(1, number_of - fixed)
        return jnp.zeros((number_of,), jnp.int32).at[order[jnp.where(places < fixed, places, moved)]].set(jnp.asarray(tallies, jnp.int32))

    tallies = jnp.where(number % 4 == 0, named(crowded, number // 4), named(usual, number - number // 4 - 1))
    mixed = jax.random.permutation(jax.random.fold_in(own, 3), number_of)
    donor, taker = mixed[0:number_of // 2 * 2:2], mixed[1:number_of // 2 * 2:2]
    slack = jnp.minimum(tallies[donor] - 1, most - tallies[taker]) // 2
    slack = jnp.where((donor == order[0]) | (taker == order[0]) | (tallies[taker] == 0), 0, jnp.maximum(slack, 0))
    moved = jax.random.randint(jax.random.fold_in(own, 4), (number_of // 2,), 0, 1 << 20) % (slack + 1)
    tallies = tallies.at[donor].add(-moved).at[taker].add(moved)
    items = jnp.searchsorted(jnp.cumsum(tallies), jnp.arange(rows * top), side="right").astype(jnp.int32)
    grid = items.reshape(top, rows).T
    grid = grid[jax.random.permutation(jax.random.fold_in(own, 1), rows)]
    rotation = jax.random.randint(jax.random.fold_in(own, 2), (rows, 1), 0, top)
    return jnp.take_along_axis(grid, (jnp.arange(top)[None, :] + rotation) % top, axis=1)


def load_shares(count, total, bound, slope, full):
    loads = [(1 << 20) // math.isqrt(grade ** slope) + 1 for grade in range(1, count + 1)]
    largest = bound if full else min(bound, max(-(-total // count), total * loads[0] // sum(loads)))
    least = 1 if total - largest >= count - 1 else 0
    holding, rest = [largest] + [least] * (count - 1), total - largest - least * (count - 1)
    while rest > 0:
        free = [i for i in range(1, count) if holding[i] < largest] or [i for i in range(1, count) if holding[i] < bound]
        mass, left = sum([loads[i] for i in free]), rest
        for i in free:
            addition = min(bound - holding[i], max(1, left * loads[i] // mass), rest)
            holding[i] = holding[i] + addition
            rest = rest - addition
    return np.array(holding)


def centred(rng, shape, width, most, pieces=(), kind=jnp.bfloat16):
    gain = levels(rng, shape, pieces, -0.22, 0.18) if pieces else 1.0
    entries = jax.random.normal(rng, shape, jnp.float32) * width * gain
    return jnp.minimum(jnp.maximum(entries, -most), most).astype(kind)


def noise_with(rng, shape, scale, limit, pieces, heavy, kind=jnp.bfloat16):
    entries = scale * jax.random.normal(rng, shape, jnp.float32)
    if pieces:
        entries = entries * levels(rng, shape, pieces, -0.22, 0.18)
    return jnp.clip(spiked(entries, jax.random.fold_in(rng, 3), *heavy), -limit, limit).astype(kind)


def setup_inputs(seed: int = 0) -> dict:
    key_list = jax.random.split(jax.random.key(seed), 15)
    expert_input = centred(key_list[0], (TOKENS, D), 1.0, 6.0, ((0, 8),))
    cotangent = noise_with(key_list[1], (TOKENS, D), 1.0, 6.0, ((0, 8),), (0, 1, 8, 2.0))
    routes_keys = jax.random.split(jax.random.fold_in(key_list[2], 1), TOKENS // TOK_DEV)
    routes_turns = jax.random.permutation(jax.random.fold_in(key_list[2], 3), TOKENS // TOK_DEV)
    routes = jax.vmap(lambda own, number: assign_block(jax.random.fold_in(key_list[2], 2), own, number, TOK_DEV, EXPERTS, TOP, CAP, 1))(routes_keys, routes_turns).reshape((TOKENS, TOP))
    route_weight = jnp.clip(jnp.exp(math.log(2.5) - 2.5257286 * jax.random.uniform(key_list[3], (TOKENS, TOP), jnp.float32) ** levels(key_list[3], (TOKENS, TOP), ((0, 8),), -0.2, 0.2)), 0.2, 2.5)
    expert_gate = centred(key_list[4], (EXPERTS, D, FF), D ** -0.5, 0.125, ((0, 8), (2, 4)))
    expert_up = centred(key_list[5], (EXPERTS, D, FF), D ** -0.5, 0.125, ((0, 8), (2, 4)))
    expert_down = centred(key_list[6], (EXPERTS, FF, D), FF ** -0.5, 0.1875, ((0, 8), (1, 4)))
    conv_out = draw_conv_out(jax.random.fold_in(key_list[14], 71), 0)
    conv_value = centred(key_list[8], (TOKENS, CW), 1.0, 6.0, ((0, 8), (1, 4)))
    conv_gate = centred(key_list[9], (TOKENS, CW), 1.0, 6.0, ((0, 8), (1, 4)))
    conv_taps = centred(key_list[10], (KW, CW), KW ** -0.5, 1.0, ((1, 4),), jnp.float32)
    norm_gain = jnp.clip(1.0 + 0.18 * jax.random.normal(key_list[11], (CW,), jnp.float32), 0.1, 1.9)
    norm_bias = centred(key_list[12], (CW,), 0.5, 3.0, ((0, 4),), jnp.float32)
    out_weight = centred(key_list[13], (CW, D), CW ** -0.5, 0.1875, ((0, 4),))
    return {"expert_input": expert_input, "cotangent": cotangent, "routes": routes, "route_weight": route_weight, "expert_gate": expert_gate, "expert_up": expert_up, "expert_down": expert_down, "conv_out": conv_out, "conv_value": conv_value, "conv_gate": conv_gate, "conv_taps": conv_taps, "norm_gain": norm_gain, "norm_bias": norm_bias, "out_weight": out_weight}


norm_eps = 1e-06

def build_slots(block_routes):
    assigns = block_routes.shape[0] * block_routes.shape[1]
    flat_routes = block_routes.reshape(assigns)
    onehot = (flat_routes[:, None] == jnp.arange(EXPERTS, dtype=jnp.int32)[None, :]).astype(jnp.int32)
    slot_rank = lax.optimization_barrier(jnp.sum((jnp.cumsum(onehot, axis=0) - onehot) * onehot, axis=1))
    target = flat_routes * CAP + slot_rank
    return jnp.full((EXPERTS * CAP,), assigns, jnp.int32).at[target].set(jnp.arange(assigns, dtype=jnp.int32))

def reference(expert_input, cotangent, routes, route_weight, expert_gate, expert_up, expert_down, conv_out, conv_value, conv_gate, conv_taps, norm_gain, norm_bias, out_weight):
    block_assigns = TOK_DEV * TOP
    slot_sets = jax.vmap(build_slots)(routes.reshape(N_SP, TOK_DEV, TOP))
    offsets = (jnp.arange(N_SP, dtype=jnp.int32) * block_assigns)[:, None]
    global_ids = jnp.where(slot_sets == block_assigns, TOKENS * TOP, slot_sets + offsets).astype(jnp.int32)
    expert_ids = global_ids.reshape(N_SP, EXPERTS, CAP).transpose(1, 0, 2).reshape(EXPERTS, N_SP * CAP)
    scaled = (cotangent.astype(jnp.float32)[:, None, :] * route_weight[:, :, None]).astype(jnp.bfloat16)
    padded_cot = jnp.concatenate([scaled.reshape(TOKENS * TOP, D), jnp.zeros((1, D), jnp.bfloat16)], axis=0)
    padded_in = jnp.concatenate([expert_input, jnp.zeros((1, D), jnp.bfloat16)], axis=0)

    def expert_step(routed, inputs):
        slot_ids, w_gate, w_up, w_down = inputs
        tokens_of = slot_ids // TOP
        slot_rows = padded_in[tokens_of]
        slot_cots = padded_cot[slot_ids]
        pre_gate = jnp.dot(slot_rows, w_gate, preferred_element_type=jnp.float32)
        pre_up = jnp.dot(slot_rows, w_up, preferred_element_type=jnp.float32)
        gate_sig = jax.nn.sigmoid(pre_gate)
        gate_act = pre_gate * gate_sig
        hidden = (gate_act * pre_up).astype(jnp.bfloat16)
        hidden_grad = jnp.dot(slot_cots, w_down.T, preferred_element_type=jnp.float32)
        down_part = jnp.dot(hidden.T, slot_cots, preferred_element_type=jnp.float32)
        gate_pre = (hidden_grad * pre_up * gate_sig * (1.0 + pre_gate * (1.0 - gate_sig))).astype(jnp.bfloat16)
        up_pre = (hidden_grad * gate_act).astype(jnp.bfloat16)
        gate_part = jnp.dot(slot_rows.T, gate_pre, preferred_element_type=jnp.float32)
        up_part = jnp.dot(slot_rows.T, up_pre, preferred_element_type=jnp.float32)
        slot_grad = jnp.zeros((slot_rows.shape[0], D), jnp.float32)
        for group_idx in range(N_TP):
            group_lo = group_idx * FGROUP
            group_hi = group_lo + FGROUP
            group_part = jnp.dot(gate_pre[:, group_lo:group_hi], w_gate[:, group_lo:group_hi].T, preferred_element_type=jnp.float32)
            group_part = group_part + jnp.dot(up_pre[:, group_lo:group_hi], w_up[:, group_lo:group_hi].T, preferred_element_type=jnp.float32)
            slot_grad = slot_grad + lax.optimization_barrier(group_part.astype(jnp.bfloat16)).astype(jnp.float32)
        rounded = lax.optimization_barrier(slot_grad.astype(jnp.bfloat16)).astype(jnp.float32)
        routed = routed.at[tokens_of].add(rounded)
        return (routed, (gate_part, up_part, down_part))
    routed, weight_grads = lax.scan(expert_step, jnp.zeros((TOKENS + 1, D), jnp.float32), (expert_ids, expert_gate, expert_up, expert_down))
    gate_grad, up_grad, down_grad = weight_grads
    resid_grad = (cotangent.astype(jnp.float32) + routed[:TOKENS]).astype(jnp.bfloat16)
    mix_grad = jnp.dot(resid_grad, out_weight.T, preferred_element_type=jnp.float32)
    conv_vals = conv_out.astype(jnp.float32)
    row_mean = lax.optimization_barrier(jnp.mean(conv_vals, axis=1, keepdims=True))
    row_var = lax.optimization_barrier(jnp.mean((conv_vals - row_mean) ** 2, axis=1, keepdims=True))
    row_rstd = lax.rsqrt(row_var + norm_eps)
    normed = (conv_vals - row_mean) * row_rstd
    norm_pre = normed * norm_gain[None, :] + norm_bias[None, :]
    norm_sig = jax.nn.sigmoid(norm_pre)
    conv_act = (norm_pre * norm_sig).astype(jnp.bfloat16)
    out_weight_grad = jnp.dot(conv_act.T, resid_grad, preferred_element_type=jnp.float32)
    norm_grad = mix_grad * norm_sig * (1.0 + norm_pre * (1.0 - norm_sig)) * norm_gain[None, :]
    grad_mean = lax.optimization_barrier(jnp.mean(norm_grad, axis=1, keepdims=True))
    grad_dot = lax.optimization_barrier(jnp.mean(norm_grad * normed, axis=1, keepdims=True))
    conv_grad = row_rstd * (norm_grad - grad_mean - normed * grad_dot)
    extended = jnp.concatenate([conv_grad, jnp.zeros((KW - 1, CW), jnp.float32)], axis=0)
    glu_grad = jnp.zeros((TOKENS, CW), jnp.float32)
    for lag_index in range(KW):
        begin = KW - 1 - lag_index
        glu_grad = glu_grad + conv_taps[lag_index][None, :] * extended[begin:begin + TOKENS]
    gate_sig = jax.nn.sigmoid(conv_gate.astype(jnp.float32))
    value_grad = (glu_grad * gate_sig).astype(jnp.bfloat16)
    gate_in_grad = (glu_grad * conv_value.astype(jnp.float32) * gate_sig * (1.0 - gate_sig)).astype(jnp.bfloat16)
    return (gate_grad, up_grad, down_grad, resid_grad, out_weight_grad, value_grad, gate_in_grad)
```

```python
import functools

import jax
import jax.numpy as jnp
from jax import lax
from jax.experimental import pallas as pl
from jax.experimental.pallas import tpu as pltpu
from jax.sharding import PartitionSpec as P

norm_eps = 1e-06
MESH = pl.DeviceIdType.MESH
bf16 = jnp.bfloat16
f32 = jnp.float32


def doublings(count):
    steps, step = [], 1
    while step < count:
        steps.append(step)
        step *= 2
    return steps


def block_order(count):
    low, high, order = 1, count - 1, []
    while low <= high:
        order.append(high)
        if low < high:
            order.append(low)
        low, high = low + 1, high - 1
    return order


def greet(me_s, me_t, sp, tp):
    barrier = pltpu.get_barrier_semaphore()
    peers = [(me_s ^ d, me_t) for d in range(1, sp)] + [(me_s, me_t ^ m) for m in doublings(tp)]
    for peer in peers:
        pl.semaphore_signal(barrier, inc=1, device_id=peer, device_id_type=MESH)
    pl.semaphore_wait(barrier, len(peers))


def remote(source, target, send_sem, recv_sem, peer):
    return pltpu.make_async_remote_copy(
        src_ref=source,
        dst_ref=target,
        send_sem=send_sem,
        recv_sem=recv_sem,
        device_id=peer,
        device_id_type=MESH,
    )


def dispatch_kernel(sp, tp, send_ref, out_ref, send_sem, recv_sem, own_sem):
    me_s, me_t = lax.axis_index("sp"), lax.axis_index("tp")
    share = send_ref.shape[-1]
    steps = doublings(tp)
    arrays = send_ref.shape[0]
    events = [(a, d) for a in range(arrays) for d in [0] + block_order(sp)]

    def cols(q):
        return pl.ds(pl.multiple_of((me_t ^ q) * share, share), share)

    greet(me_s, me_t, sp, tp)
    copies = {}
    for i, (a, d) in enumerate(events):
        if d:
            copies[0, i] = remote(
                send_ref.at[a, me_s ^ d],
                out_ref.at[a, me_s, :, cols(0)],
                send_sem.at[0, i],
                recv_sem.at[0, i],
                (me_s ^ d, me_t),
            )
        else:
            copies[0, i] = pltpu.make_async_copy(
                send_ref.at[a, me_s], out_ref.at[a, me_s, :, cols(0)], own_sem.at[a]
            )
        copies[0, i].start()

    def forward(i, q, m):
        a, d = events[i]
        place = out_ref.at[a, me_s ^ d, :, cols(q)]
        source = send_ref.at[a, me_s] if d == 0 and q == 0 else place
        copies[q ^ m, i] = remote(
            source, place, send_sem.at[q ^ m, i], recv_sem.at[q ^ m, i], (me_s, me_t ^ m)
        )
        copies[q ^ m, i].start()

    def relay(i):
        for low in reversed(steps[1:]):
            for q in range(low, tp, 2 * low):
                copies[q, i].wait_recv()
                for m in reversed(steps):
                    if m < low:
                        forward(i, q, m)

    lag = 2
    for i, (a, d) in enumerate(events):
        if d:
            copies[0, i].wait_recv()
        for m in reversed(steps):
            forward(i, 0, m)
        if i >= lag:
            relay(i - lag)
    for i in range(max(0, len(events) - lag), len(events)):
        relay(i)
    for i, (a, d) in enumerate(events):
        for q in range(1, tp, 2):
            copies[q, i].wait_recv()
        for q in range(tp):
            if q or d:
                copies[q, i].wait_send()
            else:
                copies[q, i].wait()


def dispatch(send, sp, tp):
    arrays, _, rows, share = send.shape
    vmem = pl.BlockSpec(memory_space=pltpu.VMEM)
    return pl.pallas_call(
        functools.partial(dispatch_kernel, sp, tp),
        out_shape=jax.ShapeDtypeStruct((arrays, sp, rows, share * tp), bf16),
        in_specs=[vmem],
        out_specs=vmem,
        scratch_shapes=[
            pltpu.SemaphoreType.DMA((tp, arrays * sp)),
            pltpu.SemaphoreType.DMA((tp, arrays * sp)),
            pltpu.SemaphoreType.DMA((arrays,)),
        ],
        compiler_params=pltpu.CompilerParams(collective_id=0, has_side_effects=True),
    )(send)


def return_kernel(
    sp,
    tp,
    part_ref,
    pick_ref,
    cot_ref,
    resid_ref,
    got_ref,
    sums_ref,
    fin_ref,
    back_ref,
    acc_ref,
    got_send,
    got_recv,
    back_send,
    back_recv,
    join_send,
    join_recv,
):
    me_s, me_t = lax.axis_index("sp"), lax.axis_index("tp")
    share = cot_ref.shape[-1]
    steps = doublings(tp)
    order = block_order(sp) + [0]
    slot, sent_slot = {}, {}
    for k, m in enumerate(steps):
        for q in range(0, tp, 2 * m):
            slot[k, q] = len(slot)
            if k:
                sent_slot[k, q ^ m] = len(sent_slot)

    def cols(q):
        return pl.ds(pl.multiple_of((me_t ^ q) * share, share), share)

    greet(me_s, me_t, sp, tp)
    copies = {}

    def give(k, q, d, source):
        m = steps[k]
        place = slot[k, q ^ m]
        copy = remote(
            source,
            got_ref.at[place, me_s ^ d],
            got_send.at[place, d],
            got_recv.at[place, d],
            (me_s, me_t ^ m),
        )
        copy.start()
        copies[k, q ^ m, d] = copy

    for d in order:
        for q in range(1, tp, 2):
            give(0, q, d, part_ref.at[me_s ^ d, :, cols(q)])

    def total(k, q, d):
        value = part_ref[me_s ^ d, :, cols(q)].astype(f32)
        for j in range(k):
            value = value + got_ref[slot[j, q], me_s ^ d].astype(f32)
        return value.astype(bf16)

    def stage(k, d):
        for q in range(0, tp, 2 * steps[k - 1]):
            copies[k - 1, q, d].wait_recv()
        if k < len(steps):
            m = steps[k]
            for q in range(m, tp, 2 * m):
                held = sums_ref.at[sent_slot[k, q], me_s ^ d]
                held[...] = total(k, q, d)
                give(k, q, d, held)
        elif d:
            fin_ref[me_s ^ d] = total(k, 0, d)
            copies["back", d] = remote(
                fin_ref.at[me_s ^ d],
                back_ref.at[me_s],
                back_send.at[d],
                back_recv.at[d],
                (me_s ^ d, me_t),
            )
            copies["back", d].start()
        else:
            back_ref[me_s] = total(k, 0, d)

    lag = 2
    depth = len(steps)
    for i in range(len(order) + lag * (depth - 1)):
        for k in range(1, depth + 1):
            at = i - lag * (k - 1)
            if 0 <= at < len(order):
                stage(k, order[at])

    acc_ref[...] = cot_ref[...].astype(f32)
    for d in [0] + order[:-1]:
        if d:
            copies["back", d].wait_recv()
        acc_ref[...] += jnp.dot(
            pick_ref[me_s ^ d], back_ref[me_s ^ d], preferred_element_type=f32
        )
    resid_ref[:, cols(0)] = acc_ref[...].astype(bf16)

    def join(q, m):
        place = resid_ref.at[:, cols(q)]
        copies["join", q ^ m] = remote(
            place, place, join_send.at[q ^ m], join_recv.at[q ^ m], (me_s, me_t ^ m)
        )
        copies["join", q ^ m].start()

    for m in reversed(steps):
        join(0, m)
    for low in reversed(steps[1:]):
        for q in range(low, tp, 2 * low):
            copies["join", q].wait_recv()
            for m in reversed(steps):
                if m < low:
                    join(q, m)
    for q in range(1, tp, 2):
        copies["join", q].wait_recv()
    for copy in copies.values():
        copy.wait_send()


def give_back(part, picks, own_cot, sp, tp):
    _, rows, width = part.shape
    tok_rows, share = own_cot.shape
    vmem = pl.BlockSpec(memory_space=pltpu.VMEM)
    spare = max(1, tp // 2 - 1)
    return pl.pallas_call(
        functools.partial(return_kernel, sp, tp),
        out_shape=jax.ShapeDtypeStruct((tok_rows, width), bf16),
        in_specs=[vmem] * 3,
        out_specs=vmem,
        scratch_shapes=[
            pltpu.VMEM((tp - 1, sp, rows, share), bf16),
            pltpu.VMEM((spare, sp, rows, share), bf16),
            pltpu.VMEM((sp, rows, share), bf16),
            pltpu.VMEM((sp, rows, share), bf16),
            pltpu.VMEM((tok_rows, share), f32),
            pltpu.SemaphoreType.DMA((tp - 1, sp)),
            pltpu.SemaphoreType.DMA((tp - 1, sp)),
            pltpu.SemaphoreType.DMA((sp,)),
            pltpu.SemaphoreType.DMA((sp,)),
            pltpu.SemaphoreType.DMA((tp,)),
            pltpu.SemaphoreType.DMA((tp,)),
        ],
        compiler_params=pltpu.CompilerParams(collective_id=1, has_side_effects=True),
    )(part, picks, own_cot)


def passed_along(value, axis, steps):
    count = lax.axis_size(axis)
    leading, last = (max(0, -steps), min(count, count - steps))
    return lax.ppermute(value, axis, [(source, source + steps) for source in range(leading, last)])


def on_device(
    expert_input,
    cotangent,
    routes,
    route_weight,
    expert_gate,
    expert_up,
    expert_down,
    conv_out,
    conv_value,
    conv_gate,
    conv_taps,
    norm_gain,
    norm_bias,
    out_weight,
):
    sp_count = lax.axis_size("sp")
    tp_count = lax.axis_size("tp")
    tok_rows, model_width = expert_input.shape
    share_cols = model_width // tp_count
    top_count = routes.shape[1]
    local_exp = expert_gate.shape[0]
    experts = local_exp * sp_count
    capacity = 3 * top_count * tok_rows // (2 * experts)
    named = routes[:, :, None] == jnp.arange(experts, dtype=jnp.int32)
    token_at = jnp.arange(tok_rows, dtype=jnp.int32)
    earlier = (token_at[:, None] > token_at[None, :]).astype(jnp.bfloat16)
    before = jnp.dot(
        earlier, jnp.any(named, axis=1).astype(jnp.bfloat16), preferred_element_type=jnp.float32
    )
    slot_rank = jnp.sum(jnp.where(named, before[:, None, :], 0.0), axis=2).astype(jnp.int32)
    target = routes * capacity + slot_rank
    rows = local_exp * capacity
    slot_at = (
        jnp.arange(sp_count, dtype=jnp.int32)[:, None, None] * rows
        + jnp.arange(rows, dtype=jnp.int32)[None, None, :]
    )
    pick = [
        (target[:, k][None, :, None] == slot_at).astype(jnp.bfloat16) for k in range(top_count)
    ]
    picks = sum(pick[1:], pick[0])
    share_at = lax.axis_index("tp") * share_cols
    own_in = lax.dynamic_slice_in_dim(expert_input, share_at, share_cols, 1)
    own_cot = lax.dynamic_slice_in_dim(cotangent, share_at, share_cols, 1)

    def chosen(which, values):
        return jnp.einsum("str,td->srd", which, values, preferred_element_type=jnp.float32)

    send_rows = chosen(picks, own_in).astype(jnp.bfloat16)
    send_cot = sum(
        chosen(
            pick[k],
            (own_cot.astype(jnp.float32) * route_weight[:, k][:, None]).astype(jnp.bfloat16),
        )
        for k in range(top_count)
    ).astype(jnp.bfloat16)
    arrived = dispatch(jnp.stack([send_rows, send_cot]), sp_count, tp_count)

    def by_expert(blocks):
        return (
            blocks.reshape(sp_count, local_exp, capacity, model_width)
            .transpose(1, 0, 2, 3)
            .reshape(local_exp, sp_count * capacity, model_width)
        )

    slot_rows = by_expert(arrived[0])
    slot_cots = by_expert(arrived[1])
    pre_gate = jnp.einsum(
        "lrd,ldf->lrf", slot_rows, expert_gate, preferred_element_type=jnp.float32
    )
    pre_up = jnp.einsum("lrd,ldf->lrf", slot_rows, expert_up, preferred_element_type=jnp.float32)
    gate_sig = jax.nn.sigmoid(pre_gate)
    gate_act = pre_gate * gate_sig
    hidden = (gate_act * pre_up).astype(jnp.bfloat16)
    hidden_grad = jnp.einsum(
        "lrd,lfd->lrf", slot_cots, expert_down, preferred_element_type=jnp.float32
    )
    down_grad = jnp.einsum("lrf,lrd->lfd", hidden, slot_cots, preferred_element_type=jnp.float32)
    gate_pre = (hidden_grad * pre_up * gate_sig * (1.0 + pre_gate * (1.0 - gate_sig))).astype(
        jnp.bfloat16
    )
    up_pre = (hidden_grad * gate_act).astype(jnp.bfloat16)
    gate_grad = jnp.einsum("lrd,lrf->ldf", slot_rows, gate_pre, preferred_element_type=jnp.float32)
    up_grad = jnp.einsum("lrd,lrf->ldf", slot_rows, up_pre, preferred_element_type=jnp.float32)
    partial_rows = jnp.einsum(
        "lrf,ldf->lrd", gate_pre, expert_gate, preferred_element_type=jnp.float32
    )
    partial_rows = partial_rows + jnp.einsum(
        "lrf,ldf->lrd", up_pre, expert_up, preferred_element_type=jnp.float32
    )
    partial_src = (
        partial_rows.reshape(local_exp, sp_count, capacity, model_width)
        .transpose(1, 0, 2, 3)
        .reshape(sp_count, rows, model_width)
    )
    partial_low = partial_src.astype(jnp.bfloat16)
    resid_grad = give_back(partial_low, picks, own_cot, sp_count, tp_count)
    mix_grad = lax.dot_general(
        resid_grad, out_weight, (((1,), (1,)), ((), ())), preferred_element_type=jnp.float32
    )
    channels = conv_out.shape[1] * tp_count
    conv_vals = conv_out.astype(jnp.float32)
    row_sum, row_square = lax.psum(
        (jnp.sum(conv_vals, axis=1), jnp.sum(conv_vals * conv_vals, axis=1)), "tp"
    )
    row_mean = (row_sum / channels)[:, None]
    row_var = (row_square / channels)[:, None] - row_mean * row_mean
    row_rstd = lax.rsqrt(row_var + norm_eps)
    normed = (conv_vals - row_mean) * row_rstd
    norm_pre = normed * norm_gain[None, :] + norm_bias[None, :]
    norm_sig = jax.nn.sigmoid(norm_pre)
    conv_act = (norm_pre * norm_sig).astype(jnp.bfloat16)
    norm_grad = mix_grad * norm_sig * (1.0 + norm_pre * (1.0 - norm_sig)) * norm_gain[None, :]
    grad_sum, grad_dot = lax.psum(
        (jnp.sum(norm_grad, axis=1), jnp.sum(norm_grad * normed, axis=1)), "tp"
    )
    conv_grad = row_rstd * (
        norm_grad - (grad_sum / channels)[:, None] - normed * (grad_dot / channels)[:, None]
    )
    taps_count = conv_taps.shape[0]
    next_rows = passed_along(conv_grad[: taps_count - 1], "sp", -1)
    extended = jnp.concatenate([conv_grad, next_rows], axis=0)
    glu_grad = jnp.zeros_like(conv_grad)
    for lag_index in range(taps_count):
        begin = taps_count - 1 - lag_index
        glu_grad = glu_grad + conv_taps[lag_index][None, :] * extended[begin : begin + tok_rows]
    gate_sig_in = jax.nn.sigmoid(conv_gate.astype(jnp.float32))
    value_grad = (glu_grad * gate_sig_in).astype(jnp.bfloat16)
    gate_in_grad = (
        glu_grad * conv_value.astype(jnp.float32) * gate_sig_in * (1.0 - gate_sig_in)
    ).astype(jnp.bfloat16)
    projected = lax.psum_scatter(
        lax.dot_general(
            resid_grad, conv_act, (((0,), (0,)), ((), ())), preferred_element_type=jnp.float32
        ).astype(jnp.bfloat16),
        "sp",
        scatter_dimension=0,
        tiled=True,
    ).astype(jnp.float32)
    out_weight_grad = projected.T
    return (gate_grad, up_grad, down_grad, resid_grad, out_weight_grad, value_grad, gate_in_grad)


def solution(mesh):
    return jax.shard_map(
        on_device,
        mesh=mesh,
        in_specs=(
            P("sp", None),
            P("sp", None),
            P("sp", None),
            P("sp", None),
            P("sp", None, "tp"),
            P("sp", None, "tp"),
            P("sp", "tp", None),
            P("sp", "tp"),
            P("sp", "tp"),
            P("sp", "tp"),
            P(None, "tp"),
            P("tp"),
            P("tp"),
            P("tp", None),
        ),
        out_specs=(
            P("sp", None, "tp"),
            P("sp", None, "tp"),
            P("sp", "tp", None),
            P("sp", None),
            P("tp", "sp"),
            P("sp", "tp"),
            P("sp", "tp"),
        ),
        check_vma=False,
    )
```

```python
import functools

import jax
import jax.numpy as jnp
from jax import lax
from jax.experimental import pallas as pl
from jax.experimental.pallas import tpu as pltpu
from jax.sharding import PartitionSpec as P

norm_eps = 1e-06
MESH = pl.DeviceIdType.MESH
bf16 = jnp.bfloat16
f32 = jnp.float32


def doublings(count):
    steps, step = [], 1
    while step < count:
        steps.append(step)
        step *= 2
    return steps


def block_order(count):
    low, high, order = 1, count - 1, []
    while low <= high:
        order.append(high)
        if low < high:
            order.append(low)
        low, high = low + 1, high - 1
    return order


def greet(me_s, me_t, sp, tp):
    barrier = pltpu.get_barrier_semaphore()
    peers = [(me_s ^ d, me_t) for d in range(1, sp)] + [(me_s, me_t ^ m) for m in doublings(tp)]
    for peer in peers:
        pl.semaphore_signal(barrier, inc=1, device_id=peer, device_id_type=MESH)
    pl.semaphore_wait(barrier, len(peers))


def remote(source, target, send_sem, recv_sem, peer):
    return pltpu.make_async_remote_copy(
        src_ref=source,
        dst_ref=target,
        send_sem=send_sem,
        recv_sem=recv_sem,
        device_id=peer,
        device_id_type=MESH,
    )


def expert_kernel(sp, tp, *refs):
    (rows_ref, cots_ref, gate_ref, up_ref, down_ref, pick_ref, cot_ref) = refs[:7]
    (resid_ref, gate_out, up_out, down_out) = refs[7:11]
    (in_ref, hid_ref, gpre_ref, upre_ref, part_ref, got_ref, sums_ref, fin_ref) = refs[11:19]
    (back_ref, acc_ref, own_sem, send_sem, recv_sem, got_send, got_recv) = refs[19:26]
    (back_send, back_recv, join_send, join_recv) = refs[26:]
    me_s, me_t = lax.axis_index("sp"), lax.axis_index("tp")
    share = cot_ref.shape[-1]
    local_exp, capacity = rows_ref.shape[1:3]
    steps = doublings(tp)
    depth = len(steps)
    order = [0] + block_order(sp)
    sent = (rows_ref, cots_ref)
    slot, sent_slot = {}, {}
    for k, m in enumerate(steps):
        for q in range(0, tp, 2 * m):
            slot[k, q] = len(slot)
            if k:
                sent_slot[k, q ^ m] = len(sent_slot)

    def cols(q):
        return pl.ds(pl.multiple_of((me_t ^ q) * share, share), share)

    greet(me_s, me_t, sp, tp)
    copies = {}

    for d in order:
        for a in range(2):
            if d:
                copy = remote(
                    sent[a].at[me_s ^ d],
                    in_ref.at[a, me_s, :, :, cols(0)],
                    send_sem.at[0, a, d],
                    recv_sem.at[0, a, d],
                    (me_s ^ d, me_t),
                )
            else:
                copy = pltpu.make_async_copy(
                    sent[a].at[me_s], in_ref.at[a, me_s, :, :, cols(0)], own_sem.at[a]
                )
            copy.start()
            copies[0, a, d] = copy

    def forward(a, d, q, m):
        place = in_ref.at[a, me_s ^ d, :, :, cols(q)]
        source = sent[a].at[me_s] if d == 0 and q == 0 else place
        copy = remote(
            source,
            place,
            send_sem.at[q ^ m, a, d],
            recv_sem.at[q ^ m, a, d],
            (me_s, me_t ^ m),
        )
        copy.start()
        copies[q ^ m, a, d] = copy

    def spread(d):
        for a in range(2):
            if d:
                copies[0, a, d].wait_recv()
            for m in reversed(steps):
                forward(a, d, 0, m)

    def relay(d):
        for a in range(2):
            for low in reversed(steps[1:]):
                for q in range(low, tp, 2 * low):
                    copies[q, a, d].wait_recv()
                    for m in reversed(steps):
                        if m < low:
                            forward(a, d, q, m)

    def give(k, q, d, source):
        m = steps[k]
        place = slot[k, q ^ m]
        copy = remote(
            source,
            got_ref.at[place, me_s ^ d],
            got_send.at[place, d],
            got_recv.at[place, d],
            (me_s, me_t ^ m),
        )
        copy.start()
        copies["got", k, q ^ m, d] = copy

    def dot(left, right, contract):
        return lax.dot_general(left, right, (contract, ((), ())), preferred_element_type=f32)

    def compute(d):
        for a in range(2):
            for q in range(1, tp, 2):
                copies[q, a, d].wait_recv()
            if d == 0:
                copies[0, a, d].wait()
        at = me_s ^ d
        for e in range(local_exp):
            slot_rows, slot_cots = in_ref[0, at, e], in_ref[1, at, e]
            pre_gate = dot(slot_rows, gate_ref[e], ((1,), (0,)))
            pre_up = dot(slot_rows, up_ref[e], ((1,), (0,)))
            hidden_grad = dot(slot_cots, down_ref[e], ((1,), (1,)))
            gate_sig = jax.nn.sigmoid(pre_gate)
            gate_act = pre_gate * gate_sig
            hid_ref[e, at] = (gate_act * pre_up).astype(bf16)
            gate_pre = (
                hidden_grad * pre_up * gate_sig * (1.0 + pre_gate * (1.0 - gate_sig))
            ).astype(bf16)
            up_pre = (hidden_grad * gate_act).astype(bf16)
            gpre_ref[e, at] = gate_pre
            upre_ref[e, at] = up_pre
            part = dot(gate_pre, gate_ref[e], ((1,), (1,)))
            part = part + dot(up_pre, up_ref[e], ((1,), (1,)))
            part_ref[at, e] = part.astype(bf16)
        for q in range(1, tp, 2):
            give(0, q, d, part_ref.at[at, :, :, cols(q)])

    def total(k, q, d):
        value = part_ref[me_s ^ d, :, :, cols(q)].astype(f32)
        for j in range(k):
            value = value + got_ref[slot[j, q], me_s ^ d].astype(f32)
        return value.astype(bf16)

    def reduce(k, d):
        for q in range(0, tp, 2 * steps[k - 1]):
            copies["got", k - 1, q, d].wait_recv()
        if k < depth:
            m = steps[k]
            for q in range(m, tp, 2 * m):
                held = sums_ref.at[sent_slot[k, q], me_s ^ d]
                held[...] = total(k, q, d)
                give(k, q, d, held)
        elif d:
            fin_ref[me_s ^ d] = total(k, 0, d)
            copy = remote(
                fin_ref.at[me_s ^ d],
                back_ref.at[me_s],
                back_send.at[d],
                back_recv.at[d],
                (me_s ^ d, me_t),
            )
            copy.start()
            copies["back", d] = copy
        else:
            back_ref[me_s] = total(k, 0, d)

    plan = [(0, spread), (1, relay), (2, compute)]
    plan += [(2 + k, functools.partial(reduce, k)) for k in range(1, depth + 1)]
    for i in range(len(order) + plan[-1][0]):
        for lag, act in plan:
            if 0 <= i - lag < len(order):
                act(order[i - lag])

    def weight_grad(e, left, right, out):
        if capacity % 16 == 0:
            whole = lambda value: value.reshape(sp * capacity, value.shape[-1])
            out[e] = dot(whole(left(slice(None))), whole(right(slice(None))), ((0,), (0,)))
        else:
            out[e] = jnp.zeros(out.shape[1:], f32)

            @pl.loop(0, sp)
            def _(at):
                out[e] += dot(left(at), right(at), ((0,), (0,)))

    for e in range(local_exp):
        weight_grad(e, lambda at: in_ref[0, at, e], lambda at: gpre_ref[e, at], gate_out)
        weight_grad(e, lambda at: in_ref[0, at, e], lambda at: upre_ref[e, at], up_out)
        weight_grad(e, lambda at: hid_ref[e, at], lambda at: in_ref[1, at, e], down_out)

    acc_ref[...] = cot_ref[...].astype(f32)
    for d in order:
        if d:
            copies["back", d].wait_recv()
        for e in range(local_exp):
            acc_ref[...] += dot(pick_ref[me_s ^ d, e], back_ref[me_s ^ d, e], ((1,), (0,)))
    resid_ref[:, cols(0)] = acc_ref[...].astype(bf16)

    def join(q, m):
        place = resid_ref.at[:, cols(q)]
        copy = remote(
            place, place, join_send.at[q ^ m], join_recv.at[q ^ m], (me_s, me_t ^ m)
        )
        copy.start()
        copies["join", q ^ m] = copy

    for m in reversed(steps):
        join(0, m)
    for low in reversed(steps[1:]):
        for q in range(low, tp, 2 * low):
            copies["join", q].wait_recv()
            for m in reversed(steps):
                if m < low:
                    join(q, m)
    for q in range(1, tp, 2):
        copies["join", q].wait_recv()
    for key, copy in copies.items():
        if not (key[0] == 0 and key[-1] == 0):
            copy.wait_send()


def run_experts(send_rows, send_cots, gate, up, down, picks, own_cot, sp, tp):
    _, local_exp, capacity, share = send_rows.shape
    width, hidden = gate.shape[1:]
    tok_rows = own_cot.shape[0]
    vmem = pl.BlockSpec(memory_space=pltpu.VMEM)
    spare = max(1, tp // 2 - 1)
    part = (sp, local_exp, capacity, share)
    kept = (local_exp, sp, capacity, hidden)
    dma = pltpu.SemaphoreType.DMA
    return pl.pallas_call(
        functools.partial(expert_kernel, sp, tp),
        out_shape=(
            jax.ShapeDtypeStruct((tok_rows, width), bf16),
            jax.ShapeDtypeStruct(gate.shape, f32),
            jax.ShapeDtypeStruct(up.shape, f32),
            jax.ShapeDtypeStruct(down.shape, f32),
        ),
        in_specs=[vmem] * 7,
        out_specs=(vmem,) * 4,
        scratch_shapes=[
            pltpu.VMEM((2, sp, local_exp, capacity, width), bf16),
            pltpu.VMEM(kept, bf16),
            pltpu.VMEM(kept, bf16),
            pltpu.VMEM(kept, bf16),
            pltpu.VMEM((sp, local_exp, capacity, width), bf16),
            pltpu.VMEM((tp - 1, *part), bf16),
            pltpu.VMEM((spare, *part), bf16),
            pltpu.VMEM(part, bf16),
            pltpu.VMEM(part, bf16),
            pltpu.VMEM((tok_rows, share), f32),
            dma((2,)),
            dma((tp, 2, sp)),
            dma((tp, 2, sp)),
            dma((tp - 1, sp)),
            dma((tp - 1, sp)),
            dma((sp,)),
            dma((sp,)),
            dma((tp,)),
            dma((tp,)),
        ],
        compiler_params=pltpu.CompilerParams(
            collective_id=0, has_side_effects=True, vmem_limit_bytes=62 * 1024 * 1024
        ),
    )(send_rows, send_cots, gate, up, down, picks, own_cot)


def passed_along(value, axis, steps):
    count = lax.axis_size(axis)
    leading, last = (max(0, -steps), min(count, count - steps))
    return lax.ppermute(value, axis, [(source, source + steps) for source in range(leading, last)])


def on_device(
    expert_input,
    cotangent,
    routes,
    route_weight,
    expert_gate,
    expert_up,
    expert_down,
    conv_out,
    conv_value,
    conv_gate,
    conv_taps,
    norm_gain,
    norm_bias,
    out_weight,
):
    sp_count = lax.axis_size("sp")
    tp_count = lax.axis_size("tp")
    tok_rows, model_width = expert_input.shape
    share_cols = model_width // tp_count
    top_count = routes.shape[1]
    local_exp = expert_gate.shape[0]
    experts = local_exp * sp_count
    capacity = 3 * top_count * tok_rows // (2 * experts)
    named = routes[:, :, None] == jnp.arange(experts, dtype=jnp.int32)
    token_at = jnp.arange(tok_rows, dtype=jnp.int32)
    earlier = (token_at[:, None] > token_at[None, :]).astype(jnp.bfloat16)
    before = jnp.dot(
        earlier, jnp.any(named, axis=1).astype(jnp.bfloat16), preferred_element_type=jnp.float32
    )
    slot_rank = jnp.sum(jnp.where(named, before[:, None, :], 0.0), axis=2).astype(jnp.int32)
    target = routes * capacity + slot_rank
    blocks = (sp_count, local_exp, tok_rows, capacity)
    slot_at = (
        lax.broadcasted_iota(jnp.int32, blocks, 0) * local_exp
        + lax.broadcasted_iota(jnp.int32, blocks, 1)
    ) * capacity + lax.broadcasted_iota(jnp.int32, blocks, 3)
    pick = [
        (target[:, k][None, None, :, None] == slot_at).astype(jnp.bfloat16) for k in range(top_count)
    ]
    picks = sum(pick[1:], pick[0])
    share_at = lax.axis_index("tp") * share_cols
    own_in = lax.dynamic_slice_in_dim(expert_input, share_at, share_cols, 1)
    own_cot = lax.dynamic_slice_in_dim(cotangent, share_at, share_cols, 1)

    def chosen(which, values):
        return jnp.einsum("setr,td->serd", which, values, preferred_element_type=jnp.float32)

    send_rows = chosen(picks, own_in).astype(jnp.bfloat16)
    send_cot = sum(
        chosen(
            pick[k],
            (own_cot.astype(jnp.float32) * route_weight[:, k][:, None]).astype(jnp.bfloat16),
        )
        for k in range(top_count)
    ).astype(jnp.bfloat16)
    resid_grad, gate_grad, up_grad, down_grad = run_experts(
        send_rows,
        send_cot,
        expert_gate,
        expert_up,
        expert_down,
        picks,
        own_cot,
        sp_count,
        tp_count,
    )
    mix_grad = lax.dot_general(
        resid_grad, out_weight, (((1,), (1,)), ((), ())), preferred_element_type=jnp.float32
    )
    channels = conv_out.shape[1] * tp_count
    conv_vals = conv_out.astype(jnp.float32)
    row_sum, row_square = lax.psum(
        (jnp.sum(conv_vals, axis=1), jnp.sum(conv_vals * conv_vals, axis=1)), "tp"
    )
    row_mean = (row_sum / channels)[:, None]
    row_var = (row_square / channels)[:, None] - row_mean * row_mean
    row_rstd = lax.rsqrt(row_var + norm_eps)
    normed = (conv_vals - row_mean) * row_rstd
    norm_pre = normed * norm_gain[None, :] + norm_bias[None, :]
    norm_sig = jax.nn.sigmoid(norm_pre)
    conv_act = (norm_pre * norm_sig).astype(jnp.bfloat16)
    norm_grad = mix_grad * norm_sig * (1.0 + norm_pre * (1.0 - norm_sig)) * norm_gain[None, :]
    grad_sum, grad_dot = lax.psum(
        (jnp.sum(norm_grad, axis=1), jnp.sum(norm_grad * normed, axis=1)), "tp"
    )
    conv_grad = row_rstd * (
        norm_grad - (grad_sum / channels)[:, None] - normed * (grad_dot / channels)[:, None]
    )
    taps_count = conv_taps.shape[0]
    next_rows = passed_along(conv_grad[: taps_count - 1], "sp", -1)
    extended = jnp.concatenate([conv_grad, next_rows], axis=0)
    glu_grad = jnp.zeros_like(conv_grad)
    for lag_index in range(taps_count):
        begin = taps_count - 1 - lag_index
        glu_grad = glu_grad + conv_taps[lag_index][None, :] * extended[begin : begin + tok_rows]
    gate_sig_in = jax.nn.sigmoid(conv_gate.astype(jnp.float32))
    value_grad = (glu_grad * gate_sig_in).astype(jnp.bfloat16)
    gate_in_grad = (
        glu_grad * conv_value.astype(jnp.float32) * gate_sig_in * (1.0 - gate_sig_in)
    ).astype(jnp.bfloat16)
    projected = lax.psum_scatter(
        lax.dot_general(
            resid_grad, conv_act, (((0,), (0,)), ((), ())), preferred_element_type=jnp.float32
        ).astype(jnp.bfloat16),
        "sp",
        scatter_dimension=0,
        tiled=True,
    ).astype(jnp.float32)
    out_weight_grad = projected.T
    return (gate_grad, up_grad, down_grad, resid_grad, out_weight_grad, value_grad, gate_in_grad)


def solution(mesh):
    return jax.shard_map(
        on_device,
        mesh=mesh,
        in_specs=(
            P("sp", None),
            P("sp", None),
            P("sp", None),
            P("sp", None),
            P("sp", None, "tp"),
            P("sp", None, "tp"),
            P("sp", "tp", None),
            P("sp", "tp"),
            P("sp", "tp"),
            P("sp", "tp"),
            P(None, "tp"),
            P("tp"),
            P("tp"),
            P("tp", None),
        ),
        out_specs=(
            P("sp", None, "tp"),
            P("sp", None, "tp"),
            P("sp", "tp", None),
            P("sp", None),
            P("tp", "sp"),
            P("sp", "tp"),
            P("sp", "tp"),
        ),
        check_vma=False,
    )
```

```python
import functools

import jax
import jax.numpy as jnp
from jax import lax
from jax.experimental import pallas as pl
from jax.experimental.pallas import tpu as pltpu
from jax.sharding import PartitionSpec as P

norm_eps = 1e-06
MESH = pl.DeviceIdType.MESH
bf16 = jnp.bfloat16
f32 = jnp.float32


def doublings(count):
    steps, step = [], 1
    while step < count:
        steps.append(step)
        step *= 2
    return steps


def block_order(count):
    low, high, order = 1, count - 1, []
    while low <= high:
        order.append(high)
        if low < high:
            order.append(low)
        low, high = low + 1, high - 1
    return order


def greet(me_s, me_t, sp, tp):
    barrier = pltpu.get_barrier_semaphore()
    peers = [(me_s ^ d, me_t) for d in range(1, sp)] + [(me_s, me_t ^ q) for q in range(1, tp)]
    for peer in peers:
        pl.semaphore_signal(barrier, inc=1, device_id=peer, device_id_type=MESH)
    pl.semaphore_wait(barrier, len(peers))


def remote(source, target, send_sem, recv_sem, peer):
    return pltpu.make_async_remote_copy(
        src_ref=source,
        dst_ref=target,
        send_sem=send_sem,
        recv_sem=recv_sem,
        device_id=peer,
        device_id_type=MESH,
    )


def two_rows(first, second):
    lane = lax.broadcasted_iota(jnp.int32, (first.shape[0], 128), 1)
    tile = jnp.where(lane == 0, first, jnp.where(lane == 1, second, 0.0))
    return tile.T[:8]


def share_sums(held_ref, send_sem, recv_sem, me_s, me_t, tp):
    copies = [
        remote(
            held_ref.at[0], held_ref.at[q], send_sem.at[q], recv_sem.at[q], (me_s, me_t ^ q)
        )
        for q in range(1, tp)
    ]
    for copy in copies:
        copy.start()
    return copies


def summed(held_ref, copies):
    value = held_ref[0]
    for q, copy in enumerate(copies, 1):
        copy.wait_recv()
        value = value + held_ref[q]
    return value


def expert_kernel(sp, tp, *refs):
    (rows_ref, cots_ref, gate_ref, up_ref, down_ref, pick_ref, cot_ref, conv_ref) = refs[:8]
    (resid_ref, gate_out, up_out, down_out, stats_out) = refs[8:13]
    refs = refs[2:]
    (in_ref, hid_ref, gpre_ref, upre_ref, part_ref, got_ref, sums_ref, fin_ref) = refs[11:19]
    (back_ref, acc_ref, own_sem, send_sem, recv_sem, got_send, got_recv) = refs[19:26]
    (back_send, back_recv, join_send, join_recv, stat_ref, stat_send, stat_recv) = refs[26:]
    me_s, me_t = lax.axis_index("sp"), lax.axis_index("tp")
    share = cot_ref.shape[-1]
    local_exp, capacity = rows_ref.shape[1:3]
    steps = doublings(tp)
    depth = len(steps)
    order = [0] + block_order(sp)
    sent = (rows_ref, cots_ref)
    slot, sent_slot = {}, {}
    for k, m in enumerate(steps):
        for q in range(0, tp, 2 * m):
            slot[k, q] = len(slot)
            if k:
                sent_slot[k, q ^ m] = len(sent_slot)

    def cols(q):
        return pl.ds(pl.multiple_of((me_t ^ q) * share, share), share)

    greet(me_s, me_t, sp, tp)
    copies = {}

    for d in order:
        for a in range(2):
            if d:
                copy = remote(
                    sent[a].at[me_s ^ d],
                    in_ref.at[a, me_s, :, :, cols(0)],
                    send_sem.at[0, a, d],
                    recv_sem.at[0, a, d],
                    (me_s ^ d, me_t),
                )
            else:
                copy = pltpu.make_async_copy(
                    sent[a].at[me_s], in_ref.at[a, me_s, :, :, cols(0)], own_sem.at[a]
                )
            copy.start()
            copies[0, a, d] = copy

    def forward(a, d, q, m):
        place = in_ref.at[a, me_s ^ d, :, :, cols(q)]
        source = sent[a].at[me_s] if d == 0 and q == 0 else place
        copy = remote(
            source,
            place,
            send_sem.at[q ^ m, a, d],
            recv_sem.at[q ^ m, a, d],
            (me_s, me_t ^ m),
        )
        copy.start()
        copies[q ^ m, a, d] = copy

    def spread(d):
        for a in range(2):
            if d:
                copies[0, a, d].wait_recv()
            for m in reversed(steps):
                forward(a, d, 0, m)

    def relay(d):
        for a in range(2):
            for low in reversed(steps[1:]):
                for q in range(low, tp, 2 * low):
                    copies[q, a, d].wait_recv()
                    for m in reversed(steps):
                        if m < low:
                            forward(a, d, q, m)

    def give(k, q, d, source):
        m = steps[k]
        place = slot[k, q ^ m]
        copy = remote(
            source,
            got_ref.at[place, me_s ^ d],
            got_send.at[place, d],
            got_recv.at[place, d],
            (me_s, me_t ^ m),
        )
        copy.start()
        copies["got", k, q ^ m, d] = copy

    def dot(left, right, contract):
        return lax.dot_general(left, right, (contract, ((), ())), preferred_element_type=f32)

    def compute(d):
        for a in range(2):
            for q in range(1, tp, 2):
                copies[q, a, d].wait_recv()
            if d == 0:
                copies[0, a, d].wait()
        at = me_s ^ d
        for e in range(local_exp):
            slot_rows, slot_cots = in_ref[0, at, e], in_ref[1, at, e]
            pre_gate = dot(slot_rows, gate_ref[e], ((1,), (0,)))
            pre_up = dot(slot_rows, up_ref[e], ((1,), (0,)))
            hidden_grad = dot(slot_cots, down_ref[e], ((1,), (1,)))
            gate_sig = jax.nn.sigmoid(pre_gate)
            gate_act = pre_gate * gate_sig
            hid_ref[e, at] = (gate_act * pre_up).astype(bf16)
            gate_pre = (
                hidden_grad * pre_up * gate_sig * (1.0 + pre_gate * (1.0 - gate_sig))
            ).astype(bf16)
            up_pre = (hidden_grad * gate_act).astype(bf16)
            gpre_ref[e, at] = gate_pre
            upre_ref[e, at] = up_pre
            part = dot(gate_pre, gate_ref[e], ((1,), (1,)))
            part = part + dot(up_pre, up_ref[e], ((1,), (1,)))
            part_ref[at, e] = part.astype(bf16)
        for q in range(1, tp, 2):
            give(0, q, d, part_ref.at[at, :, :, cols(q)])

    def total(k, q, d):
        value = part_ref[me_s ^ d, :, :, cols(q)].astype(f32)
        for j in range(k):
            value = value + got_ref[slot[j, q], me_s ^ d].astype(f32)
        return value.astype(bf16)

    def reduce(k, d):
        for q in range(0, tp, 2 * steps[k - 1]):
            copies["got", k - 1, q, d].wait_recv()
        if k < depth:
            m = steps[k]
            for q in range(m, tp, 2 * m):
                held = sums_ref.at[sent_slot[k, q], me_s ^ d]
                held[...] = total(k, q, d)
                give(k, q, d, held)
        elif d:
            fin_ref[me_s ^ d] = total(k, 0, d)
            copy = remote(
                fin_ref.at[me_s ^ d],
                back_ref.at[me_s],
                back_send.at[d],
                back_recv.at[d],
                (me_s ^ d, me_t),
            )
            copy.start()
            copies["back", d] = copy
        else:
            back_ref[me_s] = total(k, 0, d)

    conv_vals = conv_ref[...].astype(f32)
    stat_ref[0] = two_rows(
        jnp.sum(conv_vals, axis=1, keepdims=True),
        jnp.sum(conv_vals * conv_vals, axis=1, keepdims=True),
    )

    plan = [(0, spread), (1, relay), (2, compute)]
    plan += [(2 + k, functools.partial(reduce, k)) for k in range(1, depth + 1)]
    stat_copies = []
    for i in range(len(order) + plan[-1][0]):
        if i == 1:
            stat_copies = share_sums(stat_ref, stat_send, stat_recv, me_s, me_t, tp)
        for lag, act in plan:
            if 0 <= i - lag < len(order):
                act(order[i - lag])

    def weight_grad(e, left, right, out):
        if capacity % 16 == 0:
            whole = lambda value: value.reshape(sp * capacity, value.shape[-1])
            out[e] = dot(whole(left(slice(None))), whole(right(slice(None))), ((0,), (0,)))
        else:
            out[e] = jnp.zeros(out.shape[1:], f32)

            @pl.loop(0, sp)
            def _(at):
                out[e] += dot(left(at), right(at), ((0,), (0,)))

    for e in range(local_exp):
        weight_grad(e, lambda at: in_ref[0, at, e], lambda at: gpre_ref[e, at], gate_out)
        weight_grad(e, lambda at: in_ref[0, at, e], lambda at: upre_ref[e, at], up_out)
        weight_grad(e, lambda at: hid_ref[e, at], lambda at: in_ref[1, at, e], down_out)

    acc_ref[...] = cot_ref[...].astype(f32)
    for d in order:
        if d:
            copies["back", d].wait_recv()
        for e in range(local_exp):
            acc_ref[...] += dot(pick_ref[me_s ^ d, e], back_ref[me_s ^ d, e], ((1,), (0,)))
    resid_ref[:, cols(0)] = acc_ref[...].astype(bf16)

    def join(q, m):
        place = resid_ref.at[:, cols(q)]
        copy = remote(
            place, place, join_send.at[q ^ m], join_recv.at[q ^ m], (me_s, me_t ^ m)
        )
        copy.start()
        copies["join", q ^ m] = copy

    for m in reversed(steps):
        join(0, m)
    for low in reversed(steps[1:]):
        for q in range(low, tp, 2 * low):
            copies["join", q].wait_recv()
            for m in reversed(steps):
                if m < low:
                    join(q, m)
    for q in range(1, tp, 2):
        copies["join", q].wait_recv()
    stats_out[...] = summed(stat_ref, stat_copies)
    for copy in stat_copies:
        copy.wait_send()
    for key, copy in copies.items():
        if not (key[0] == 0 and key[-1] == 0):
            copy.wait_send()


def run_experts(send_rows, send_cots, gate, up, down, picks, own_cot, conv_out, sp, tp):
    _, local_exp, capacity, share = send_rows.shape
    width, hidden = gate.shape[1:]
    tok_rows = own_cot.shape[0]
    vmem = pl.BlockSpec(memory_space=pltpu.VMEM)
    spare = max(1, tp // 2 - 1)
    part = (sp, local_exp, capacity, share)
    kept = (local_exp, sp, capacity, hidden)
    dma = pltpu.SemaphoreType.DMA
    return pl.pallas_call(
        functools.partial(expert_kernel, sp, tp),
        out_shape=(
            jax.ShapeDtypeStruct((tok_rows, width), bf16),
            jax.ShapeDtypeStruct(gate.shape, f32),
            jax.ShapeDtypeStruct(up.shape, f32),
            jax.ShapeDtypeStruct(down.shape, f32),
            jax.ShapeDtypeStruct((8, tok_rows), f32),
        ),
        in_specs=[vmem] * 8,
        out_specs=(vmem,) * 5,
        scratch_shapes=[
            pltpu.VMEM((2, sp, local_exp, capacity, width), bf16),
            pltpu.VMEM(kept, bf16),
            pltpu.VMEM(kept, bf16),
            pltpu.VMEM(kept, bf16),
            pltpu.VMEM((sp, local_exp, capacity, width), bf16),
            pltpu.VMEM((tp - 1, *part), bf16),
            pltpu.VMEM((spare, *part), bf16),
            pltpu.VMEM(part, bf16),
            pltpu.VMEM(part, bf16),
            pltpu.VMEM((tok_rows, share), f32),
            dma((2,)),
            dma((tp, 2, sp)),
            dma((tp, 2, sp)),
            dma((tp - 1, sp)),
            dma((tp - 1, sp)),
            dma((sp,)),
            dma((sp,)),
            dma((tp,)),
            dma((tp,)),
            pltpu.VMEM((tp, 8, tok_rows), f32),
            dma((tp,)),
            dma((tp,)),
        ],
        compiler_params=pltpu.CompilerParams(
            collective_id=0, has_side_effects=True, vmem_limit_bytes=62 * 1024 * 1024
        ),
    )(send_rows, send_cots, gate, up, down, picks, own_cot, conv_out)


def conv_kernel(sp, tp, *refs):
    (resid_ref, stats_ref, conv_ref, value_ref, gate_ref, taps_ref) = refs[:6]
    (gain_ref, bias_ref, weight_ref) = refs[6:9]
    (weight_out, value_out, gate_out) = refs[9:12]
    (proj_ref, low_ref, near_ref, sum_ref, far_ref, ext_ref, halo_ref, stat_ref) = refs[12:20]
    (near_send, near_recv, far_send, far_recv) = refs[20:24]
    (halo_send, halo_recv, stat_send, stat_recv) = refs[24:]
    me_s, me_t = lax.axis_index("sp"), lax.axis_index("tp")
    tok_rows, own_channels = conv_ref.shape
    channels = own_channels * tp
    taps_count = taps_ref.shape[0]
    halo_rows = halo_ref.shape[0]
    pairs = min(2, sp)
    order = [d for d in block_order(sp) if d % pairs == 0] + [0]

    greet(me_s, me_t, sp, tp)

    totals = stats_ref[...].T / channels
    row_mean = totals[:, 0:1]
    row_rstd = lax.rsqrt(totals[:, 1:2] - row_mean * row_mean + norm_eps)
    normed = (conv_ref[...].astype(f32) - row_mean) * row_rstd
    norm_pre = normed * gain_ref[...] + bias_ref[...]
    norm_sig = jax.nn.sigmoid(norm_pre)
    conv_act = (norm_pre * norm_sig).astype(bf16)
    projected = lax.dot_general(
        resid_ref[...], conv_act, (((0,), (0,)), ((), ())), preferred_element_type=f32
    )
    proj_ref[...] = projected.reshape(proj_ref.shape)
    low_ref[...] = proj_ref[...].astype(bf16)

    near, far = {}, {}
    if pairs == 2:
        for d in order:
            near[d] = remote(
                low_ref.at[me_s ^ 1 ^ d],
                near_ref.at[d // 2],
                near_send.at[d // 2],
                near_recv.at[d // 2],
                (me_s ^ 1, me_t),
            )
            near[d].start()

    def pass_on(d):
        near[d].wait_recv()
        if d:
            sum_ref[d // 2] = (proj_ref[me_s ^ d] + near_ref[d // 2].astype(f32)).astype(bf16)
            far[d] = remote(
                sum_ref.at[d // 2],
                far_ref.at[d // 2],
                far_send.at[d // 2],
                far_recv.at[d // 2],
                (me_s ^ d, me_t),
            )
            far[d].start()

    mix_grad = lax.dot_general(
        resid_ref[...], weight_ref[...], (((1,), (1,)), ((), ())), preferred_element_type=f32
    )
    norm_grad = mix_grad * norm_sig * (1.0 + norm_pre * (1.0 - norm_sig)) * gain_ref[...]
    stat_ref[0] = two_rows(
        jnp.sum(norm_grad, axis=1, keepdims=True),
        jnp.sum(norm_grad * normed, axis=1, keepdims=True),
    )
    stat_copies = share_sums(stat_ref, stat_send, stat_recv, me_s, me_t, tp)
    means = summed(stat_ref, stat_copies).T / channels
    ext_ref[0:tok_rows, :] = row_rstd * (norm_grad - means[:, 0:1] - normed * means[:, 1:2])
    halo = remote(
        ext_ref.at[0:halo_rows, :],
        halo_ref,
        halo_send,
        halo_recv,
        (lax.rem(me_s + sp - 1, sp), me_t),
    )
    halo.start()

    chunk = 64 if tok_rows % 64 == 0 else tok_rows
    starts = list(range(0, tok_rows, chunk))

    def convolve(start):
        glu_grad = jnp.zeros((chunk, own_channels), f32)
        for lag_index in range(taps_count):
            begin = start + taps_count - 1 - lag_index
            glu_grad = glu_grad + taps_ref[lag_index, :][None, :] * ext_ref[
                begin : begin + chunk, :
            ]
        at = slice(start, start + chunk)
        gate_sig = jax.nn.sigmoid(gate_ref[at, :].astype(f32))
        value_out[at, :] = (glu_grad * gate_sig).astype(bf16)
        gate_out[at, :] = (
            glu_grad * value_ref[at, :].astype(f32) * gate_sig * (1.0 - gate_sig)
        ).astype(bf16)

    early = [start for start in starts if start + chunk + taps_count - 1 <= tok_rows]
    for i in range(max(len(order), len(early))):
        if i < len(order) and pairs == 2:
            pass_on(order[i])
        if i < len(early):
            convolve(early[i])
    halo.wait_recv()
    ext_ref[tok_rows : tok_rows + halo_rows, :] = jnp.where(me_s == sp - 1, 0.0, halo_ref[...])
    for start in starts[len(early) :]:
        convolve(start)

    total = proj_ref[me_s]
    if pairs == 2:
        total = total + near_ref[0].astype(f32)
    for d in order[:-1]:
        far[d].wait_recv()
        total = total + far_ref[d // 2].astype(f32)
    weight_out[...] = total
    for copy in [halo, *stat_copies, *near.values(), *far.values()]:
        copy.wait_send()


def run_conv(resid, stats, conv, value, gate, taps, gain, bias, weight, sp, tp):
    tok_rows, own_channels = conv.shape
    share = resid.shape[1] // sp
    vmem = pl.BlockSpec(memory_space=pltpu.VMEM)
    dma = pltpu.SemaphoreType.DMA
    half = max(1, sp // 2)
    halo_rows = -(-(taps.shape[0] - 1) // 8) * 8
    return pl.pallas_call(
        functools.partial(conv_kernel, sp, tp),
        out_shape=(
            jax.ShapeDtypeStruct((share, own_channels), f32),
            jax.ShapeDtypeStruct(conv.shape, bf16),
            jax.ShapeDtypeStruct(conv.shape, bf16),
        ),
        in_specs=[vmem] * 9,
        out_specs=(vmem,) * 3,
        scratch_shapes=[
            pltpu.VMEM((sp, share, own_channels), f32),
            pltpu.VMEM((sp, share, own_channels), bf16),
            pltpu.VMEM((half, share, own_channels), bf16),
            pltpu.VMEM((half, share, own_channels), bf16),
            pltpu.VMEM((half, share, own_channels), bf16),
            pltpu.VMEM((tok_rows + halo_rows, own_channels), f32),
            pltpu.VMEM((halo_rows, own_channels), f32),
            pltpu.VMEM((tp, 8, tok_rows), f32),
            dma((half,)),
            dma((half,)),
            dma((half,)),
            dma((half,)),
            dma(()),
            dma(()),
            dma((tp,)),
            dma((tp,)),
        ],
        compiler_params=pltpu.CompilerParams(
            collective_id=1, has_side_effects=True, vmem_limit_bytes=40 * 1024 * 1024
        ),
    )(resid, stats, conv, value, gate, taps, gain, bias, weight)


def on_device(
    expert_input,
    cotangent,
    routes,
    route_weight,
    expert_gate,
    expert_up,
    expert_down,
    conv_out,
    conv_value,
    conv_gate,
    conv_taps,
    norm_gain,
    norm_bias,
    out_weight,
):
    sp_count = lax.axis_size("sp")
    tp_count = lax.axis_size("tp")
    tok_rows, model_width = expert_input.shape
    share_cols = model_width // tp_count
    top_count = routes.shape[1]
    local_exp = expert_gate.shape[0]
    experts = local_exp * sp_count
    capacity = 3 * top_count * tok_rows // (2 * experts)
    named = routes[:, :, None] == jnp.arange(experts, dtype=jnp.int32)
    token_at = jnp.arange(tok_rows, dtype=jnp.int32)
    earlier = (token_at[:, None] > token_at[None, :]).astype(jnp.bfloat16)
    before = jnp.dot(
        earlier, jnp.any(named, axis=1).astype(jnp.bfloat16), preferred_element_type=jnp.float32
    )
    slot_rank = jnp.sum(jnp.where(named, before[:, None, :], 0.0), axis=2).astype(jnp.int32)
    target = routes * capacity + slot_rank
    blocks = (sp_count, local_exp, tok_rows, capacity)
    slot_at = (
        lax.broadcasted_iota(jnp.int32, blocks, 0) * local_exp
        + lax.broadcasted_iota(jnp.int32, blocks, 1)
    ) * capacity + lax.broadcasted_iota(jnp.int32, blocks, 3)
    pick = [
        (target[:, k][None, None, :, None] == slot_at).astype(jnp.bfloat16) for k in range(top_count)
    ]
    picks = sum(pick[1:], pick[0])
    share_at = lax.axis_index("tp") * share_cols
    own_in = lax.dynamic_slice_in_dim(expert_input, share_at, share_cols, 1)
    own_cot = lax.dynamic_slice_in_dim(cotangent, share_at, share_cols, 1)

    def chosen(which, values):
        return jnp.einsum("setr,td->serd", which, values, preferred_element_type=jnp.float32)

    send_rows = chosen(picks, own_in).astype(jnp.bfloat16)
    send_cot = sum(
        chosen(
            pick[k],
            (own_cot.astype(jnp.float32) * route_weight[:, k][:, None]).astype(jnp.bfloat16),
        )
        for k in range(top_count)
    ).astype(jnp.bfloat16)
    resid_grad, gate_grad, up_grad, down_grad, row_stats = run_experts(
        send_rows,
        send_cot,
        expert_gate,
        expert_up,
        expert_down,
        picks,
        own_cot,
        conv_out,
        sp_count,
        tp_count,
    )
    projected, value_grad, gate_in_grad = run_conv(
        resid_grad,
        row_stats,
        conv_out,
        conv_value,
        conv_gate,
        conv_taps,
        norm_gain[None, :],
        norm_bias[None, :],
        out_weight,
        sp_count,
        tp_count,
    )
    out_weight_grad = projected.T
    return (gate_grad, up_grad, down_grad, resid_grad, out_weight_grad, value_grad, gate_in_grad)


def solution(mesh):
    return jax.shard_map(
        on_device,
        mesh=mesh,
        in_specs=(
            P("sp", None),
            P("sp", None),
            P("sp", None),
            P("sp", None),
            P("sp", None, "tp"),
            P("sp", None, "tp"),
            P("sp", "tp", None),
            P("sp", "tp"),
            P("sp", "tp"),
            P("sp", "tp"),
            P(None, "tp"),
            P("tp"),
            P("tp"),
            P("tp", None),
        ),
        out_specs=(
            P("sp", None, "tp"),
            P("sp", None, "tp"),
            P("sp", "tp", None),
            P("sp", None),
            P("tp", "sp"),
            P("sp", "tp"),
            P("sp", "tp"),
        ),
        check_vma=False,
    )
```
